32 devices in a mesh: sp: 16 (over z, y, core), tp: 2 (over x).
Axes of the slice: x: 2, y: 2, z: 4, core: 2. Of those that a mesh axis runs over, the one named last changes fastest.
Arguments:
- queries: bfloat16 [8192, 1024], P('sp', 'tp'), may hold values from -160 to 160
- keys: bfloat16 [8192, 256], P('sp', 'tp'), may hold values from -5 to 5
- values: bfloat16 [8192, 256], P('sp', 'tp'), may hold values from -6 to 6
- doc_ids: int32 [8192], P('sp'), may hold values from 0 to 7, never falling along the last dimension, each value on 1 to 2048 neighbouring positions
- sink_logit: float32 [16], P('tp'), may hold values from 1 to 6
- w_out: bfloat16 [1024, 2048], P('tp'), may hold values from -0.1875 to 0.1875
- residual: bfloat16 [8192, 2048], P(('sp', 'tp')), may hold values from -6 to 6
- ffn_gain: float32 [2048], replicated, may hold values from 0.1 to 1.9
- expert_ids: int32 [8192, 8], P(('sp', 'tp')), may hold values from 0 to 15, all different within a row; in each aligned block of 128 rows (0 to 127, 128 to 255, ...) at most 96 rows name the same one
- expert_weight: float32 [8192, 8], P(('sp', 'tp')), may hold values from 0.2 to 2
- exp_gate: bfloat16 [16, 2048, 512], P('sp'), may hold values from -0.125 to 0.125
- exp_up: bfloat16 [16, 2048, 512], P('sp'), may hold values from -0.125 to 0.125
- exp_down: bfloat16 [16, 512, 2048], P('sp'), may hold values from -0.25 to 0.25
- shared_gate: bfloat16 [2048, 512], P(None, 'tp'), may hold values from -0.125 to 0.125
- shared_up: bfloat16 [2048, 512], P(None, 'tp'), may hold values from -0.125 to 0.125
- shared_down: bfloat16 [512, 2048], P('tp'), may hold values from -0.25 to 0.25
Outputs:
- output: bfloat16 [8192, 2048], P(('sp', 'tp'))
The draws below stay inside these ranges and needn't reach their ends.
Inputs may be any that keep to these rules, and one draw needn't show every extreme that they name: `doc_ids`: never falling along the sequence; every document holds at most 2048 positions, and one holds exactly that many. `expert_ids`: each row names 8 different experts. In each aligned block of 128 rows no expert is named by more than 96 rows, and in some blocks one expert is named by exactly 96 rows.
All inputs are finite; a program needn't handle non-finite values.
Results may differ from the reference program's by a relative error of at most 0.018.
Values may be sent and summed in bfloat16 or wider, within the bound.
No kernel may reach another device: no remote copies, remote signals or barrier semaphores. Data moves between devices by JAX's collectives and lax.ppermute only.
A program may use at most 128 MiB of HBM per device.

```python
import math
import jax
import jax.numpy as jnp
import numpy as np
from jax import lax

D = 2048
HQ = 16
KV = 4
HD = 64
WINDOW = 128
FF = 512
SFF = 512
TOP_K = 8
TOK_DEV = 512
ATTN_W = 1024
TOKENS = 8192
HALF = 128
EXPERTS = 16
CAP = 96
DOCS = 8
N_TP = 2


def drawn_pair(key):
    base_keys = jnp.clip(jax.random.normal(jax.random.fold_in(key, 101), (TOKENS, KV, HD), jnp.float32), -5.0, 5.0)
    return base_keys


def draw_keys(key, part):
    base_keys = drawn_pair(key)
    result = base_keys
    return result.reshape(TOKENS, KV * HD).astype(jnp.bfloat16)


def draw_queries(key, part):
    drawn_rows = jnp.clip(jax.random.normal(jax.random.fold_in(key, 105), (TOKENS, HQ * HD), jnp.float32), -5.0, 5.0)
    result = drawn_rows
    return result.astype(jnp.bfloat16)


def block_scale(stream_key, extent, cuts, smallest, high):
    factor_of, own = 1.0, jax.random.fold_in(stream_key, 6)
    for axis_at, parts in cuts:
        heights = jnp.exp(jax.random.uniform(jax.random.fold_in(own, axis_at), (parts,), jnp.float32, smallest / len(cuts), high / len(cuts)))
        factor_of = factor_of * jnp.repeat(heights, extent[axis_at] // parts).reshape([-1 if axis == axis_at else 1 for axis in range(len(extent))])
    return factor_of


def split_up(count, total, bound, lean):
    loads = [(1 << 20) // math.isqrt(rank ** lean) + 1 for rank in range(2, count + 1)]
    rest, given = total - bound - (count - 1), [1] * (count - 1)
    while rest > 0:
        free = [i for i in range(count - 1) if given[i] < bound]
        whole, budget = sum([loads[i] for i in free]), rest
        for i in free:
            extra = min(bound - given[i], max(1, budget * loads[i] // whole), rest)
            given[i] = given[i] + extra
            rest = rest - extra
    return np.array([bound] + given)


def uneven_parts(rng, count, total, limit, lean):
    if count == 2:
        one = jax.random.randint(rng, (), max(1, total - limit), min(limit, total - 1) + 1)
        return jnp.stack([one, total - one])
    lengths = jnp.asarray(split_up(count, total, limit, lean), jnp.int32)
    pairs = (count - 1) // 2
    source_of, receiver = lengths[1:1 + 2 * pairs:2], lengths[2:2 + 2 * pairs:2]
    slack = jnp.minimum(source_of - 1, limit - receiver)
    moved = jax.random.randint(jax.random.fold_in(rng, 1), (pairs,), 0, 1 << 20) % (slack + 1)
    lengths = lengths.at[1:1 + 2 * pairs:2].set(source_of - moved).at[2:2 + 2 * pairs:2].set(receiver + moved)
    return lengths[jax.random.permutation(jax.random.fold_in(rng, 2), count)]


def routed_block(key, own, number, rows, number_of, top, bound, lean):
    ranking = jax.random.permutation(key, number_of)
    packed, common = shares(number_of, rows * top, bound, lean, True), shares(number_of, rows * top, bound, lean, False)
    places = jnp.arange(number_of)

    def named(sizes, turn):
        used = int((sizes > 0).sum())
        fixed = max(1, used // 4)
        passed = fixed + (places - fixed + turn * (used - fixed)) % max(1, number_of - fixed)
        return jnp.zeros((number_of,), jnp.int32).at[ranking[jnp.where(places < fixed, places, passed)]].set(jnp.asarray(sizes, jnp.int32))

    sizes = jnp.where(number % 4 == 0, named(packed, number // 4), named(common, number - number // 4 - 1))
    mixed = jax.random.permutation(jax.random.fold_in(own, 3), number_of)
    donor, sink = mixed[0:number_of // 2 * 2:2], mixed[1:number_of // 2 * 2:2]
    room = jnp.minimum(sizes[donor] - 1, bound - sizes[sink]) // 2
    room = jnp.where((donor == ranking[0]) | (sink == ranking[0]) | (sizes[sink] == 0), 0, jnp.maximum(room, 0))
    passed = jax.random.randint(jax.random.fold_in(own, 4), (number_of // 2,), 0, 1 << 20) % (room + 1)
    sizes = sizes.at[donor].add(-passed).at[sink].add(passed)
    members = jnp.searchsorted(jnp.cumsum(sizes), jnp.arange(rows * top), side="right").astype(jnp.int32)
    listing = members.reshape(top, rows).T
    listing = listing[jax.random.permutation(jax.random.fold_in(own, 1), rows)]
    turn = jax.random.randint(jax.random.fold_in(own, 2), (rows, 1), 0, top)
    return jnp.take_along_axis(listing, (jnp.arange(top)[None, :] + turn) % top, axis=1)


def shares(amount, total, reach, skew, full):
    weights = [(1 << 20) // math.isqrt(grade ** skew) + 1 for grade in range(1, amount + 1)]
    largest = reach if full else min(reach, max(-(-total // amount), total * weights[0] // sum(weights)))
    least = 1 if total - largest >= amount - 1 else 0
    given, surplus = [largest] + [least] * (amount - 1), total - largest - least * (amount - 1)
    while surplus > 0:
        candidates = [i for i in range(1, amount) if given[i] < largest] or [i for i in range(1, amount) if given[i] < reach]
        pool, budget = sum([weights[i] for i in candidates]), surplus
        for i in candidates:
            more = min(reach - given[i], max(1, budget * weights[i] // pool), surplus)
            given[i] = given[i] + more
            surplus = surplus - more
    return np.array(given)


def centred(key, extent, deviation, limit, shards=(), kind=jnp.bfloat16):
    values = deviation * jax.random.normal(key, extent, jnp.float32)
    if shards:
        values = values * block_scale(key, extent, shards, -0.22, 0.18)
    return jnp.clip(values, -limit, limit).astype(kind)


def setup_inputs(seed: int = 0) -> dict:
    splits = jax.random.split(jax.random.key(seed), 17)
    queries = draw_queries(jax.random.fold_in(splits[16], 71), 0)
    keys = draw_keys(jax.random.fold_in(splits[16], 71), 0)
    values = centred(splits[2], (TOKENS, KV * HD), 1.0, 6.0, ((0, 16), (1, 2)))
    doc_ids = jnp.searchsorted(jnp.cumsum(uneven_parts(splits[3], DOCS, TOKENS, 4 * TOK_DEV, 2)), jnp.arange(TOKENS), side="right").astype(jnp.int32)
    sink_logit = jnp.clip(1.0 + 5.0 * jax.random.uniform(splits[4], (HQ,), jnp.float32) ** block_scale(splits[4], (HQ,), ((0, 2),), -0.2, 0.2), 1.0, 6.0)
    w_out = centred(splits[5], (ATTN_W, D), ATTN_W ** -0.5, 0.1875, ((0, 2),))
    residual = centred(splits[6], (TOKENS, D), 1.0, 6.0, ((0, 32),))
    ffn_gain = jnp.clip(1.0 + 0.18 * jax.random.normal(splits[7], (D,), jnp.float32), 0.1, 1.9)
    expert_ids_keys = jax.random.split(jax.random.fold_in(splits[8], 1), TOKENS // HALF)
    expert_ids_turns = jax.random.permutation(jax.random.fold_in(splits[8], 3), TOKENS // HALF)
    expert_ids = jax.vmap(lambda own, number: routed_block(jax.random.fold_in(splits[8], 2), own, number, HALF, EXPERTS, TOP_K, CAP, 2))(expert_ids_keys, expert_ids_turns).reshape((TOKENS, TOP_K))
    expert_weight = jnp.clip(jnp.exp(math.log(2.0) - 2.3025851 * jax.random.uniform(splits[9], (TOKENS, TOP_K), jnp.float32) ** block_scale(splits[9], (TOKENS, TOP_K), ((0, 32),), -0.2, 0.2)), 0.2, 2.0)
    exp_gate = centred(splits[10], (EXPERTS, D, FF), D ** -0.5, 0.125, ((0, 16),))
    exp_up = centred(splits[11], (EXPERTS, D, FF), D ** -0.5, 0.125, ((0, 16),))
    exp_down = centred(splits[12], (EXPERTS, FF, D), FF ** -0.5, 0.25, ((0, 16),))
    shared_gate = centred(splits[13], (D, SFF), D ** -0.5, 0.125, ((1, 2),))
    shared_up = centred(splits[14], (D, SFF), D ** -0.5, 0.125, ((1, 2),))
    shared_down = centred(splits[15], (SFF, D), SFF ** -0.5, 0.25, ((0, 2),))
    return dict(queries=queries, keys=keys, values=values, doc_ids=doc_ids, sink_logit=sink_logit, w_out=w_out, residual=residual, ffn_gain=ffn_gain, expert_ids=expert_ids, expert_weight=expert_weight, exp_gate=exp_gate, exp_up=exp_up, exp_down=exp_down, shared_gate=shared_gate, shared_up=shared_up, shared_down=shared_down)


norm_eps = 1e-06

def band_blocks(padded, width):
    span_count = padded.shape[0] // width - 2
    shaped = padded.reshape((span_count + 2, width) + padded.shape[1:])
    return jnp.concatenate([shaped[0:span_count:2], shaped[1:span_count + 1:2], shaped[2:span_count + 2:2], shaped[3:span_count + 3:2]], axis=1)

def reference(queries, keys, values, doc_ids, sink_logit, w_out, residual, ffn_gain, expert_ids, expert_weight, exp_gate, exp_up, exp_down, shared_gate, shared_up, shared_down):
    group_size = HQ // KV
    query_span = 2 * WINDOW
    block_count = TOKENS // query_span
    pad_rows = ((WINDOW, WINDOW), (0, 0))
    key_blocks = band_blocks(jnp.pad(keys, pad_rows), WINDOW).reshape(block_count, 4 * WINDOW, KV, HD)
    value_blocks = band_blocks(jnp.pad(values, pad_rows), WINDOW).reshape(block_count, 4 * WINDOW, KV, HD)
    marks = (doc_ids + 1).astype(jnp.int32)
    mark_blocks = band_blocks(jnp.pad(marks, (WINDOW, WINDOW)), WINDOW)
    query_blocks = queries.reshape(block_count, query_span, KV, group_size, HD)
    query_marks = marks.reshape(block_count, query_span)
    offset = jnp.arange(query_span, dtype=jnp.int32)[:, None] - jnp.arange(4 * WINDOW, dtype=jnp.int32)[None, :] + WINDOW
    near = jnp.abs(offset) <= WINDOW
    sink_term = sink_logit.astype(jnp.float32).reshape(KV, group_size)[:, :, None, None]

    def attend_block(inputs):
        query_in, key_in, value_in, key_marks, row_marks = inputs
        scores = jnp.einsum('qkgd,mkd->kgqm', query_in.astype(jnp.float32), key_in.astype(jnp.float32)) * HD ** (-0.5)
        allowed = near & (key_marks[None, :] == row_marks[:, None])
        scores = jnp.where(allowed[None, None], scores, -jnp.inf)
        row_max = jnp.maximum(lax.optimization_barrier(jnp.max(scores, axis=-1, keepdims=True)), sink_term)
        exp_scores = jnp.exp(scores - row_max)
        attn_probs = (exp_scores / (lax.optimization_barrier(jnp.sum(exp_scores, axis=-1, keepdims=True)) + jnp.exp(sink_term - row_max))).astype(jnp.bfloat16)
        result = jnp.einsum('kgqm,mkd->qkgd', attn_probs.astype(jnp.float32), value_in.astype(jnp.float32))
        return result.astype(jnp.bfloat16).reshape(query_span, HQ * HD)
    attended = lax.map(attend_block, (query_blocks, key_blocks, value_blocks, mark_blocks, query_marks)).reshape(TOKENS, HQ * HD)
    mixed = jnp.dot(attended, w_out, preferred_element_type=jnp.float32)
    resid = (residual.astype(jnp.float32) + mixed).astype(jnp.bfloat16)
    resid_f = resid.astype(jnp.float32)
    normed = (resid_f * lax.rsqrt(lax.optimization_barrier(jnp.mean(resid_f * resid_f, axis=-1, keepdims=True)) + norm_eps) * ffn_gain.astype(jnp.float32)).astype(jnp.bfloat16)
    shared_hidden = (jax.nn.silu(jnp.dot(normed, shared_gate, preferred_element_type=jnp.float32)) * jnp.dot(normed, shared_up, preferred_element_type=jnp.float32)).astype(jnp.bfloat16)
    block_units = SFF // N_TP
    shared_out = jnp.zeros((TOKENS, D), jnp.float32)
    for unit_block in range(N_TP):
        lower = unit_block * block_units
        partial_out = jnp.dot(shared_hidden[:, lower:lower + block_units], shared_down[lower:lower + block_units], preferred_element_type=jnp.float32)
        shared_out = shared_out + lax.optimization_barrier(partial_out.astype(jnp.bfloat16)).astype(jnp.float32)
    assign_count = TOKENS * TOP_K
    row_block = 512
    flat_ids = expert_ids.reshape(assign_count).astype(jnp.int32)
    order = jnp.argsort(flat_ids, stable=True).astype(jnp.int32)
    sorted_ids = flat_ids[order]
    counts = jnp.bincount(flat_ids, length=EXPERTS).astype(jnp.int32)
    starts = (jnp.cumsum(counts) - counts).astype(jnp.int32)
    padded = ((counts + row_block - 1) // row_block * row_block).astype(jnp.int32)
    ends = jnp.cumsum(padded).astype(jnp.int32)
    pad_starts = (ends - padded).astype(jnp.int32)
    dest = (pad_starts[sorted_ids] + jnp.arange(assign_count, dtype=jnp.int32) - starts[sorted_ids]).astype(jnp.int32)
    block_total = -(-assign_count // row_block) + EXPERTS
    row_source = jnp.full((block_total * row_block,), assign_count, jnp.int32).at[dest].set(order)
    block_expert = jnp.minimum(jnp.searchsorted(ends, jnp.arange(block_total, dtype=jnp.int32) * row_block, side='right'), EXPERTS - 1).astype(jnp.int32)
    flat_weight = expert_weight.reshape(assign_count).astype(jnp.float32)

    def expert_step(running, inputs):
        sources, expert_index = inputs
        live = sources < assign_count
        safe = jnp.minimum(sources, assign_count - 1)
        token_rows = (safe // TOP_K).astype(jnp.int32)
        gathered = normed[token_rows]
        hidden = (jax.nn.silu(jnp.dot(gathered, exp_gate[expert_index], preferred_element_type=jnp.float32)) * jnp.dot(gathered, exp_up[expert_index], preferred_element_type=jnp.float32)).astype(jnp.bfloat16)
        produced = jnp.dot(hidden, exp_down[expert_index], preferred_element_type=jnp.float32).astype(jnp.bfloat16)
        scale = jnp.where(live, flat_weight[safe], jnp.zeros_like(flat_weight[safe]))
        return (running.at[token_rows].add(scale[:, None] * produced.astype(jnp.float32)), None)
    routed, _ = lax.scan(expert_step, jnp.zeros((TOKENS, D), jnp.float32), (row_source.reshape(block_total, row_block), block_expert))
    return (resid.astype(jnp.float32) + shared_out + routed).astype(jnp.bfloat16)
```

```python
import functools
import math

import jax
import jax.numpy as jnp
from jax import lax
from jax.experimental import pallas as pl
from jax.experimental.pallas import tpu as pltpu
from jax.sharding import PartitionSpec as P

HD = 64
WINDOW = 128


norm_eps = 1e-06


def band_blocks(padded, width):
    span_count = padded.shape[0] // width - 2
    shaped = padded.reshape((span_count + 2, width) + padded.shape[1:])
    return jnp.concatenate(
        [
            shaped[0:span_count:2],
            shaped[1 : span_count + 1 : 2],
            shaped[2 : span_count + 2 : 2],
            shaped[3 : span_count + 3 : 2],
        ],
        axis=1,
    )


def attend(queries, ext_keys, ext_values, ext_marks, own_marks, sink_logit):
    tok_count = queries.shape[0]
    head_count = sink_logit.shape[0]
    key_heads = ext_keys.shape[1] // HD
    group_size = head_count // key_heads
    query_span = 2 * WINDOW
    block_count = tok_count // query_span
    query_blocks = queries.reshape(block_count, query_span, key_heads, group_size, HD)
    key_blocks = band_blocks(ext_keys, WINDOW).reshape(block_count, 4 * WINDOW, key_heads, HD)
    value_blocks = band_blocks(ext_values, WINDOW).reshape(block_count, 4 * WINDOW, key_heads, HD)
    mark_blocks = band_blocks(ext_marks, WINDOW)
    query_marks = own_marks.reshape(block_count, query_span)
    scores = jnp.einsum(
        "nqkgd,nmkd->nkgqm", query_blocks, key_blocks, preferred_element_type=jnp.float32
    ) * HD ** (-0.5)
    offset = (
        jnp.arange(query_span, dtype=jnp.int32)[:, None]
        - jnp.arange(4 * WINDOW, dtype=jnp.int32)[None, :]
        + WINDOW
    )
    allowed = (jnp.abs(offset) <= WINDOW)[None] & (
        mark_blocks[:, None, :] == query_marks[:, :, None]
    )
    scores = jnp.where(allowed[:, None, None], scores, -jnp.inf)
    sink_term = sink_logit.reshape(key_heads, group_size)[None, :, :, None, None]
    row_max = jnp.maximum(jnp.max(scores, axis=-1, keepdims=True), sink_term)
    exp_scores = jnp.exp(scores - row_max)
    attn_probs = (
        exp_scores / (jnp.sum(exp_scores, axis=-1, keepdims=True) + jnp.exp(sink_term - row_max))
    ).astype(jnp.bfloat16)
    result = jnp.einsum(
        "nkgqm,nmkd->nqkgd", attn_probs, value_blocks, preferred_element_type=jnp.float32
    )
    return result.astype(jnp.bfloat16).reshape(tok_count, head_count * HD)


def with_halo(keys, values, marks):
    count = lax.axis_size("sp")
    width = keys.shape[1] + values.shape[1]
    both = jnp.concatenate([keys, values], axis=1)

    def packed(rows, mark):
        line = jnp.pad(mark[None, :], ((0, 15), (0, width - WINDOW)))
        return jnp.concatenate([rows, line], axis=0)

    before = lax.ppermute(
        packed(both[-WINDOW:], marks[-WINDOW:]), "sp", [(i, i + 1) for i in range(count - 1)]
    )
    after = lax.ppermute(
        packed(both[:WINDOW], marks[:WINDOW]), "sp", [(i + 1, i) for i in range(count - 1)]
    )
    ext = jnp.concatenate([before[:WINDOW], both, after[:WINDOW]], axis=0)
    ext_marks = jnp.concatenate([before[WINDOW, :WINDOW], marks, after[WINDOW, :WINDOW]])
    return ext[:, : keys.shape[1]], ext[:, keys.shape[1] :], ext_marks


def expert_body(n_blocks, n_experts, swapped, *refs):
    flag = refs[0]
    xs = refs[1 : 1 + n_blocks]
    weight = refs[1 + n_blocks]
    mats = refs[2 + n_blocks : 2 + n_blocks + 3 * n_experts]
    outs = refs[2 + n_blocks + 3 * n_experts : 2 + 2 * n_blocks + 3 * n_experts]
    x_buf, a_buf, b_buf, d_buf, acc, x_sem, w_sem = refs[2 + 2 * n_blocks + 3 * n_experts :]
    rows = x_buf.shape[0] // n_blocks
    bufs = (a_buf, b_buf, d_buf)

    def copies(e):
        return [
            pltpu.make_async_copy(mats[3 * e + m], bufs[m].at[e % 2], w_sem.at[e % 2, m])
            for m in range(3)
        ]

    loads = [
        pltpu.make_async_copy(xs[n], x_buf.at[pl.ds(n * rows, rows)], x_sem.at[n])
        for n in range(n_blocks)
    ]
    for load in loads:
        load.start()
    pending = copies(0)
    for c in pending:
        c.start()
    for load in loads:
        load.wait()
    for e in range(n_experts):
        current = pending
        if e + 1 < n_experts:
            pending = copies(e + 1)
            for c in pending:
                c.start()
        current[0].wait()
        a = jnp.dot(x_buf[...], a_buf[e % 2], preferred_element_type=jnp.float32)
        current[1].wait()
        b = jnp.dot(x_buf[...], b_buf[e % 2], preferred_element_type=jnp.float32)
        if swapped[e]:
            turn = flag[0] == 1
            a, b = jnp.where(turn, b, a), jnp.where(turn, a, b)
        hidden = (a / (1.0 + jnp.exp(-a)) * b).astype(jnp.bfloat16)
        current[2].wait()
        made = jnp.dot(hidden, d_buf[e % 2], preferred_element_type=jnp.float32)
        part = weight[:, e : e + 1] * made.astype(jnp.bfloat16).astype(jnp.float32)
        if e == 0:
            acc[...] = part
        else:
            acc[...] += part
    for n in range(n_blocks):
        outs[n][...] = acc[n * rows : (n + 1) * rows].astype(jnp.bfloat16)


def run_experts(flag, blocks, weights, experts, swapped):
    n_blocks, n_experts = len(blocks), len(experts)
    rows, width = blocks[0].shape
    hidden = experts[0][0].shape[1]
    weight = jnp.concatenate(weights, axis=0)
    any_spec = pl.BlockSpec(memory_space=pl.ANY)
    vmem_spec = pl.BlockSpec(memory_space=pltpu.VMEM)
    flat = [m for expert in experts for m in expert]
    return pl.pallas_call(
        functools.partial(expert_body, n_blocks, n_experts, swapped),
        in_specs=[pl.BlockSpec(memory_space=pltpu.SMEM)]
        + [any_spec] * n_blocks
        + [vmem_spec]
        + [any_spec] * len(flat),
        out_specs=[vmem_spec] * n_blocks,
        out_shape=[jax.ShapeDtypeStruct((rows, width), jnp.bfloat16)] * n_blocks,
        scratch_shapes=[
            pltpu.VMEM((n_blocks * rows, width), jnp.bfloat16),
            pltpu.VMEM((2, width, hidden), jnp.bfloat16),
            pltpu.VMEM((2, width, hidden), jnp.bfloat16),
            pltpu.VMEM((2, hidden, width), jnp.bfloat16),
            pltpu.VMEM((n_blocks * rows, width), jnp.float32),
            pltpu.SemaphoreType.DMA((n_blocks,)),
            pltpu.SemaphoreType.DMA((2, 3)),
        ],
        cost_estimate=pl.CostEstimate(
            flops=6 * n_blocks * rows * width * hidden * n_experts,
            bytes_accessed=6 * width * hidden * n_experts,
            transcendentals=n_blocks * rows * hidden * n_experts,
        ),
        name="experts",
    )(flag, *blocks, weight, *flat)


def shards(
    queries,
    keys,
    values,
    doc_ids,
    sink_logit,
    w_out,
    residual,
    ffn_gain,
    expert_ids,
    expert_weight,
    exp_gate,
    exp_up,
    exp_down,
    shared_gate,
    shared_up,
    shared_down,
):
    sp, tp = lax.axis_size("sp"), lax.axis_size("tp")
    plane = 1 << (sp.bit_length() // 2)
    depth = sp // plane
    here, turn = lax.axis_index("sp"), lax.axis_index("tp")
    level, spot = here // plane, here % plane
    lane = here % 2
    row_count = residual.shape[0]

    def along_tp(value, d):
        return lax.ppermute(value, "tp", [(i, i ^ d) for i in range(tp)])

    def in_plane(value, d):
        return lax.ppermute(value, "sp", [(i, i ^ d) for i in range(sp)])

    def in_depth(value, pairs):
        return lax.ppermute(
            value, "sp", [(a * plane + g, b * plane + g) for a, b in pairs for g in range(plane)]
        )

    def swap_depth(value, d):
        return in_depth(value, [(a, a ^ d) for a in range(depth)])

    def my_half(value, axis):
        half = value.shape[axis] // 2
        return lax.dynamic_slice_in_dim(value, lane * half, half, axis)

    def other_half(value, axis):
        half = value.shape[axis] // 2
        return lax.dynamic_slice_in_dim(value, (1 - lane) * half, half, axis)

    marks = (doc_ids + 1).astype(jnp.bfloat16)
    ext_keys, ext_values, ext_marks = with_halo(keys, values, marks)

    out_mine = [along_tp(my_half(w_out, 0), d) for d in range(1, tp)]
    out_rest = [in_plane(part, 1) for part in out_mine]

    routing = jnp.concatenate([expert_ids.astype(jnp.float32), expert_weight], axis=1)
    routings = [routing] + [swap_depth(routing, d) for d in range(1, depth)]

    own = (exp_gate[0], exp_up[0], exp_down[0])
    experts, swapped = [own], [False]
    if plane == 4 and tp == 2:
        first = in_plane(jnp.where(turn == 0, own[0], own[1]), 2)
        down = in_plane(own[2], 2)
        second = along_tp(first, 1)
        across = (first, second, down)
        experts.append(tuple(in_plane(m, 1) for m in own))
        experts.append(across)
        experts.append(tuple(in_plane(m, 1) for m in across))
        swapped += [False, True, True]
    else:
        for d in range(1, plane):
            experts.append(tuple(in_plane(m, d) for m in own))
            swapped.append(False)
    flag = turn.astype(jnp.int32).reshape(1)

    def dense_weights(routing):
        top = expert_ids.shape[1]
        cols = []
        for d in range(plane):
            name = (level * plane + (spot ^ d)).astype(jnp.float32)
            cols.append(
                jnp.sum(
                    jnp.where(routing[:, :top] == name, routing[:, top:], 0.0),
                    axis=1,
                    keepdims=True,
                )
            )
        return jnp.concatenate(cols, axis=1)

    dense = [dense_weights(r) for r in routings]

    attended = attend(queries, ext_keys, ext_values, ext_marks, marks, sink_logit)
    att_own = lax.dynamic_slice_in_dim(attended, turn * row_count, row_count, 0)
    mixed = jnp.dot(att_own, w_out, preferred_element_type=jnp.float32)
    for d in range(1, tp):
        part = along_tp(
            lax.dynamic_slice_in_dim(attended, (turn ^ d) * row_count, row_count, 0), d
        )
        mixed += jnp.dot(my_half(part, 1), out_mine[d - 1], preferred_element_type=jnp.float32)
        mixed += jnp.dot(other_half(part, 1), out_rest[d - 1], preferred_element_type=jnp.float32)
    resid = (residual.astype(jnp.float32) + mixed).astype(jnp.bfloat16)
    resid_f = resid.astype(jnp.float32)
    normed = (
        resid_f
        * lax.rsqrt(jnp.mean(resid_f * resid_f, axis=-1, keepdims=True) + norm_eps)
        * ffn_gain
    ).astype(jnp.bfloat16)

    near = swap_depth(normed, 1)
    far = swap_depth(normed, 2)
    if depth == 4:
        held, far_held = lax.optimization_barrier((normed, far))
        last = in_depth(held, [(1, 2), (2, 1)]) + in_depth(far_held, [(2, 3), (1, 0)])
        arrived = [near, far, last]
    else:
        arrived = [near, far] + [swap_depth(normed, d) for d in range(3, depth)]

    shared = [(shared_gate, shared_up, shared_down)]
    for d in range(1, tp):
        part = (
            along_tp(my_half(shared_gate, 1), d),
            along_tp(my_half(shared_up, 1), d),
            along_tp(my_half(shared_down, 0), d),
        )
        shared.append(part)
        shared.append(tuple(in_plane(m, 1) for m in part))
    total = resid.astype(jnp.float32)
    for gate, up, down in shared:
        hid = (
            jax.nn.silu(jnp.dot(normed, gate, preferred_element_type=jnp.float32))
            * jnp.dot(normed, up, preferred_element_type=jnp.float32)
        ).astype(jnp.bfloat16)
        total += jnp.dot(hid, down, preferred_element_type=jnp.float32)

    (p_own,) = run_experts(flag, [normed], dense[:1], experts, swapped)
    if depth == 4:
        p_near, p_far = run_experts(flag, arrived[:2], dense[1:3], experts, swapped)
        back = [in_depth(p_far, [(0, 2), (3, 1)]), swap_depth(p_near, 1)]
        (p_last,) = run_experts(flag, arrived[2:], dense[3:], experts, swapped)
        merged = in_depth(p_last, [(3, 2), (0, 1)])
        back.append(in_depth(p_last, [(1, 2), (2, 1)]))
        relayed = (p_far.astype(jnp.float32) + merged.astype(jnp.float32)).astype(jnp.bfloat16)
        back.append(in_depth(relayed, [(2, 0), (1, 3)]))
    else:
        back = []
        for d in range(1, depth):
            (made,) = run_experts(flag, arrived[d - 1 : d], dense[d : d + 1], experts, swapped)
            back.append(swap_depth(made, d))
    total += p_own.astype(jnp.float32)
    for part in back:
        total += part.astype(jnp.float32)
    return total.astype(jnp.bfloat16)


def solution(mesh):
    placed = (
        P("sp", "tp"),
        P("sp", "tp"),
        P("sp", "tp"),
        P("sp"),
        P("tp"),
        P("tp", None),
        P(("sp", "tp"), None),
        P(),
        P(("sp", "tp"), None),
        P(("sp", "tp"), None),
        P("sp", None, None),
        P("sp", None, None),
        P("sp", None, None),
        P(None, "tp"),
        P(None, "tp"),
        P("tp", None),
    )
    return jax.shard_map(
        shards, mesh=mesh, in_specs=placed, out_specs=P(("sp", "tp"), None), check_vma=False
    )
```
